32 devices in a mesh: kv: 4 (over y, x), tp: 8 (over z, core).
Axes of the slice: x: 2, y: 2, z: 4, core: 2. Of those that a mesh axis runs over, the one named last changes fastest.
Arguments:
- tokens: bfloat16 [16, 2048], P(None, 'kv'), may hold values from -40 to 40
- lengths: int32 [16], replicated, may hold values from 1 to 4096, 19456 in all
- cache_keys: bfloat16 [16, 4096, 16, 128], P(None, 'kv', 'tp'), may hold values from -200 to 200
- cache_values: bfloat16 [16, 4096, 16, 128], P(None, 'kv', 'tp'), may hold values from -6 to 6
- lambdas: float32 [16], P('tp'), may hold values from 0.3 to 0.8
- head_gain: bfloat16 [128], replicated, may hold values from 0.099609375 to 1.8984375
- attn_gain: bfloat16 [2048], P('kv'), may hold values from 0.099609375 to 1.8984375
- w_query: bfloat16 [2048, 2048], P('kv', 'tp'), may hold values from -0.125 to 0.125
- w_key: bfloat16 [2048, 2048], P('kv', 'tp'), may hold values from -0.5 to 0.5
- w_value: bfloat16 [2048, 2048], P('kv', 'tp'), may hold values from -0.125 to 0.125
- w_out: bfloat16 [2048, 2048], P('tp', 'kv'), may hold values from -0.125 to 0.125
- first_gain: bfloat16 [2048], P('kv'), may hold values from 0.099609375 to 1.8984375
- first_gate: bfloat16 [2048, 5632], P('kv', 'tp'), may hold values from -0.125 to 0.125
- first_up: bfloat16 [2048, 5632], P('kv', 'tp'), may hold values from -0.125 to 0.125
- first_down: bfloat16 [5632, 2048], P('tp', 'kv'), may hold values from -0.078125 to 0.078125
- second_gain: bfloat16 [2048], P('kv'), may hold values from 0.099609375 to 1.8984375
- second_gate: bfloat16 [2048, 5632], P('kv', 'tp'), may hold values from -0.125 to 0.125
- second_up: bfloat16 [2048, 5632], P('kv', 'tp'), may hold values from -0.125 to 0.125
- second_down: bfloat16 [5632, 2048], P('tp', 'kv'), may hold values from -0.078125 to 0.078125
Outputs:
- stream_out: bfloat16 [16, 2048], P(None, 'kv')
The draws below stay inside these ranges and needn't reach their ends.
Inputs may be any that keep to these rules, and one draw needn't show every extreme that they name: `lengths`: one sequence has exactly 4096 live positions.
All inputs are finite; a program needn't handle non-finite values.
Results may differ from the reference program's by a relative error of at most 0.02.
Values may be sent and summed in bfloat16 or wider, within the bound.
A program may use at most 64 MiB of HBM per device.

```python
import math
import jax
import jax.numpy as jnp
import numpy as np
from jax import lax

D = 2048
FF = 5632
HEADS = 16
DK = 64
DV = 128
SEQS = 16
LENGTH = 4096


def draw_tokens(key, part):
    columns = jnp.arange(D, dtype=jnp.float32) / D
    col_scale = 0.5 * jnp.exp(math.log(4.0) * columns)[None, :]
    base = jnp.clip(jax.random.normal(key, (SEQS, D), jnp.float32), -6.0, 6.0)
    return (base * col_scale).astype(jnp.bfloat16)


def draw_cache_keys(key, part):
    shape_all = (SEQS, LENGTH, HEADS, 2 * DK)
    base = jnp.clip(jax.random.normal(key, shape_all, jnp.float32) * 1.75, -10.0, 10.0)
    return base.astype(jnp.bfloat16)


def steps_of(stream_key, dims, shards, low, largest):
    level = 1.0
    for dim, shards_of in shards:
        draws = jax.random.uniform(jax.random.fold_in(jax.random.fold_in(stream_key, 6), dim), (shards_of,), jnp.float32, low / len(shards), largest / len(shards))
        level = level * jnp.repeat(jnp.exp(draws), dims[dim] // shards_of).reshape((-1,) + (1,) * (len(dims) - 1 - dim))
    return level


def profile(number_of, total, reach, skew):
    portions = [(1 << 20) // math.isqrt(rank ** skew) + 1 for rank in range(2, number_of + 1)]
    surplus, counts = total - reach - (number_of - 1), [1] * (number_of - 1)
    while surplus > 0:
        candidates = [i for i in range(number_of - 1) if counts[i] < reach]
        pool, left = sum([portions[i] for i in candidates]), surplus
        for i in candidates:
            more = min(reach - counts[i], max(1, left * portions[i] // pool), surplus)
            counts[i] = counts[i] + more
            surplus = surplus - more
    return np.array([reach] + counts)


def uneven_parts(own_key, number_of, total, most, slope):
    if number_of == 2:
        one = jax.random.randint(own_key, (), max(1, total - most), min(most, total - 1) + 1)
        return jnp.stack([one, total - one])
    tallies = jnp.asarray(profile(number_of, total, most, slope), jnp.int32)
    pairs = (number_of - 1) // 2
    giver, sink = tallies[1:1 + 2 * pairs:2], tallies[2:2 + 2 * pairs:2]
    slack = jnp.minimum(giver - 1, most - sink)
    moved = jax.random.randint(jax.random.fold_in(own_key, 1), (pairs,), 0, 1 << 20) % (slack + 1)
    tallies = tallies.at[1:1 + 2 * pairs:2].set(giver - moved).at[2:2 + 2 * pairs:2].set(sink + moved)
    return tallies[jax.random.permutation(jax.random.fold_in(own_key, 2), number_of)]


def gaussian(own_key, extent, spread, limit, cuts=(), kind=jnp.bfloat16):
    entries = jax.random.normal(own_key, extent, jnp.float32) * spread
    if len(cuts) > 0:
        entries = steps_of(own_key, extent, cuts, -0.22, 0.18) * entries
    return jnp.clip(entries, min=-limit, max=limit).astype(kind)


def setup_inputs(seed: int = 0) -> dict:
    arg_keys = jax.random.split(jax.random.key(seed), 20)
    tokens = draw_tokens(jax.random.fold_in(arg_keys[19], 71), 0)
    lengths = uneven_parts(arg_keys[1], SEQS, LENGTH + (SEQS - 1) * (LENGTH // 4), LENGTH, 2).astype(jnp.int32)
    cache_keys = draw_cache_keys(jax.random.fold_in(arg_keys[19], 71), 0)
    cache_values = gaussian(arg_keys[3], (SEQS, LENGTH, HEADS, DV), 1.0, 6.0, ((1, 4), (2, 8)))
    lambdas = jnp.clip(0.3 + 0.5 * jax.random.uniform(arg_keys[4], (HEADS,), jnp.float32) ** steps_of(arg_keys[4], (HEADS,), ((0, 8),), -0.2, 0.2), 0.3, 0.8)
    head_gain = jnp.clip(1.0 + 0.18 * jax.random.normal(arg_keys[5], (DV,), jnp.float32), 0.099609375, 1.8984375).astype(jnp.bfloat16)
    attn_gain = jnp.clip(1.0 + 0.18 * jax.random.normal(arg_keys[6], (D,), jnp.float32), 0.099609375, 1.8984375).astype(jnp.bfloat16)
    w_query = gaussian(arg_keys[7], (D, HEADS * 2 * DK), D ** -0.5, 0.125, ((0, 4), (1, 8)))
    w_key = gaussian(arg_keys[8], (D, HEADS * 2 * DK), (D // 16) ** -0.5, 0.5, ((0, 4), (1, 8)))
    w_value = gaussian(arg_keys[9], (D, HEADS * DV), D ** -0.5, 0.125, ((0, 4), (1, 8)))
    w_out = gaussian(arg_keys[10], (HEADS * DV, D), (HEADS * DV) ** -0.5, 0.125, ((0, 8), (1, 4)))
    first_gain = jnp.clip(1.0 + 0.18 * jax.random.normal(arg_keys[11], (D,), jnp.float32), 0.099609375, 1.8984375).astype(jnp.bfloat16)
    first_gate = gaussian(arg_keys[12], (D, FF), D ** -0.5, 0.125, ((0, 4), (1, 8)))
    first_up = gaussian(arg_keys[13], (D, FF), D ** -0.5, 0.125, ((0, 4), (1, 8)))
    first_down = gaussian(arg_keys[14], (FF, D), FF ** -0.5, 0.078125, ((0, 8), (1, 4)))
    second_gain = jnp.clip(1.0 + 0.18 * jax.random.normal(arg_keys[15], (D,), jnp.float32), 0.099609375, 1.8984375).astype(jnp.bfloat16)
    second_gate = gaussian(arg_keys[16], (D, FF), D ** -0.5, 0.125, ((0, 4), (1, 8)))
    second_up = gaussian(arg_keys[17], (D, FF), D ** -0.5, 0.125, ((0, 4), (1, 8)))
    second_down = gaussian(arg_keys[18], (FF, D), FF ** -0.5, 0.078125, ((0, 8), (1, 4)))
    return {"tokens": tokens, "lengths": lengths, "cache_keys": cache_keys, "cache_values": cache_values, "lambdas": lambdas, "head_gain": head_gain, "attn_gain": attn_gain, "w_query": w_query, "w_key": w_key, "w_value": w_value, "w_out": w_out, "first_gain": first_gain, "first_gate": first_gate, "first_up": first_up, "first_down": first_down, "second_gain": second_gain, "second_gate": second_gate, "second_up": second_up, "second_down": second_down}


EPSILON = 1e-06
ROTARY_BASE = 10000.0
OUTPUT_KEEP = 0.8

def rotate(vectors, positions):
    half_width = vectors.shape[-1] // 2
    inv_freq = jnp.power(ROTARY_BASE, -jnp.arange(half_width, dtype=jnp.float32) / half_width)
    angles = positions.astype(jnp.float32)[:, None] * inv_freq[None, :]
    bcast_shape = (angles.shape[0],) + (1,) * (vectors.ndim - 2) + (half_width,)
    cosine = jnp.cos(angles).reshape(bcast_shape)
    sine_part = jnp.sin(angles).reshape(bcast_shape)
    first_half = vectors[..., :half_width]
    second_half = vectors[..., half_width:]
    return jnp.concatenate([first_half * cosine - second_half * sine_part, second_half * cosine + first_half * sine_part], axis=-1)

def channel_mix(stream, gain, w_gate, w_up, w_down):
    stream_f = stream.astype(jnp.float32)
    scaled = (stream_f * gain.astype(jnp.float32)).astype(jnp.bfloat16)
    row_scale = lax.rsqrt(lax.optimization_barrier(jnp.mean(stream_f * stream_f, axis=1, keepdims=True)) + EPSILON)
    gate = row_scale * jnp.dot(scaled, w_gate, preferred_element_type=jnp.float32)
    up_val = row_scale * jnp.dot(scaled, w_up, preferred_element_type=jnp.float32)
    hidden = (jax.nn.silu(gate) * up_val).astype(jnp.bfloat16)
    return (stream_f + 0.5 * jnp.dot(hidden, w_down, preferred_element_type=jnp.float32)).astype(jnp.bfloat16)

def reference(tokens, lengths, cache_keys, cache_values, lambdas, head_gain, attn_gain, w_query, w_key, w_value, w_out, first_gain, first_gate, first_up, first_down, second_gain, second_gate, second_up, second_down):
    first = channel_mix(tokens, first_gain, first_gate, first_up, first_down)
    seq_count = first.shape[0]
    stream_f = first.astype(jnp.float32)
    scaled = (stream_f * attn_gain.astype(jnp.float32)).astype(jnp.bfloat16)
    row_scale = lax.rsqrt(lax.optimization_barrier(jnp.mean(stream_f * stream_f, axis=1, keepdims=True)) + EPSILON)
    query = row_scale * jnp.dot(scaled, w_query, preferred_element_type=jnp.float32)
    key_new = row_scale * jnp.dot(scaled, w_key, preferred_element_type=jnp.float32)
    value_new = (row_scale * jnp.dot(scaled, w_value, preferred_element_type=jnp.float32)).astype(jnp.bfloat16)
    query = rotate(query.reshape(seq_count, HEADS, 2, DK), lengths).astype(jnp.bfloat16)
    key_new = rotate(key_new.reshape(seq_count, HEADS, 2, DK), lengths).astype(jnp.bfloat16)
    value_new = value_new.reshape(seq_count, HEADS, DV)
    live_mask = jnp.arange(LENGTH, dtype=jnp.int32)[None, :] < lengths[:, None]
    scale_att = DK ** (-0.5)

    def one_head(inputs):
        index, lam_value = inputs
        key_rows = lax.dynamic_index_in_dim(cache_keys, index, axis=2, keepdims=False).reshape(seq_count, LENGTH, 2, DK).astype(jnp.float32)
        value_rows = lax.dynamic_index_in_dim(cache_values, index, axis=2, keepdims=False).astype(jnp.float32)
        query_h = lax.dynamic_index_in_dim(query, index, axis=1, keepdims=False).astype(jnp.float32)
        key_h = lax.dynamic_index_in_dim(key_new, index, axis=1, keepdims=False).astype(jnp.float32)
        value_h = lax.dynamic_index_in_dim(value_new, index, axis=1, keepdims=False).astype(jnp.float32)
        scores = jnp.einsum('bcd,blcd->bcl', query_h, key_rows, precision=lax.Precision.HIGHEST) * scale_att
        scores = jnp.where(live_mask[:, None, :], scores, -jnp.inf)
        own_score = lax.optimization_barrier(jnp.sum(query_h * key_h, axis=2)) * scale_att
        peak_max = jnp.maximum(lax.optimization_barrier(jnp.max(scores, axis=2)), own_score)
        weights = jnp.exp(scores - peak_max[..., None])
        fresh_weight = jnp.exp(own_score - peak_max)
        denominator = lax.optimization_barrier(jnp.sum(weights, axis=2)) + fresh_weight
        rounded = lax.optimization_barrier(weights.astype(jnp.bfloat16)).astype(jnp.float32)
        summed = jnp.einsum('bcl,bld->bcd', rounded, value_rows, precision=lax.Precision.HIGHEST) + fresh_weight[..., None] * value_h[:, None, :]
        mixed = summed / denominator[..., None]
        return mixed[:, 0] - lam_value * mixed[:, 1]
    heads_out = lax.map(one_head, (jnp.arange(HEADS, dtype=jnp.int32), lambdas))
    heads_out = jnp.moveaxis(heads_out, 0, 1)
    norm_scale = lax.rsqrt(lax.optimization_barrier(jnp.mean(heads_out * heads_out, axis=2, keepdims=True)) + EPSILON)
    normed = (heads_out * norm_scale * head_gain.astype(jnp.float32) * OUTPUT_KEEP).astype(jnp.bfloat16)
    normed = normed.reshape(seq_count, HEADS * DV)
    second = (stream_f + jnp.dot(normed, w_out, preferred_element_type=jnp.float32)).astype(jnp.bfloat16)
    return channel_mix(second, second_gain, second_gate, second_up, second_down)
```

```python
import functools

import jax
import jax.numpy as jnp
import numpy as np
from jax import lax
from jax.experimental import pallas as pl
from jax.experimental.pallas import tpu as pltpu
from jax.sharding import PartitionSpec as P

EPSILON = 1e-06
ROTARY_BASE = 10000.0
OUTPUT_KEEP = 0.8
MASKED_SCORE = -1e30
F32 = jnp.float32
BF16 = jnp.bfloat16
MESH = pl.DeviceIdType.MESH
AHEAD = 2


def turned(left, right):
    return lax.dot_general(left, right, (((1,), (1,)), ((), ())), preferred_element_type=F32)


def partners(n):
    return range(n - 1, 0, -1)


def flipped(me, mask):
    other = me
    bit = 1
    while bit <= mask:
        if mask & bit:
            other = other + bit * (1 - 2 * lax.rem(lax.div(me, bit), 2))
        bit *= 2
    return other


def kernel(
    n_kv,
    n_tp,
    width,
    tokens_hbm,
    lengths_hbm,
    keys_hbm,
    values_hbm,
    lambdas_hbm,
    head_gain_hbm,
    attn_gain_hbm,
    wq_hbm,
    wk_hbm,
    wv_hbm,
    wo_hbm,
    first_gain_hbm,
    fg_hbm,
    fu_hbm,
    fd_hbm,
    second_gain_hbm,
    sg_hbm,
    su_hbm,
    sd_hbm,
    inv_freq_hbm,
    out_ref,
    tokens,
    keys,
    values,
    wq,
    wk,
    wv,
    wo,
    fg,
    fu,
    fd,
    sg,
    su,
    sd,
    head_gain,
    attn_gain,
    first_gain,
    second_gain,
    inv_freq,
    lengths,
    lambdas,
    mix1,
    mix2,
    down1,
    down2,
    proj,
    qnew,
    knew,
    vnew,
    part,
    stat,
    own_part,
    qrows,
    load_sem,
    kv_send,
    kv_recv,
    tp_send,
    tp_recv,
):
    me_kv = lax.axis_index("kv")
    me_tp = lax.axis_index("tp")
    seqs, cols = tokens.shape
    units = fg.shape[0]
    pad = mix1.shape[-1]
    heads = wq.shape[1] // 128
    rows = 2 * heads

    loads = {}
    for number, (name, source, target) in enumerate(
        (
            ("tokens", tokens_hbm, tokens),
            ("first_gain", first_gain_hbm, first_gain),
            ("fg", fg_hbm, fg),
            ("fu", fu_hbm, fu),
            ("fd", fd_hbm, fd),
            ("lengths", lengths_hbm, lengths),
            ("inv_freq", inv_freq_hbm, inv_freq),
            ("attn_gain", attn_gain_hbm, attn_gain),
            ("wq", wq_hbm, wq),
            ("wk", wk_hbm, wk),
            ("wv", wv_hbm, wv),
            ("keys", keys_hbm, keys),
            ("values", values_hbm, values),
            ("lambdas", lambdas_hbm, lambdas),
            ("head_gain", head_gain_hbm, head_gain),
            ("wo", wo_hbm, wo),
            ("second_gain", second_gain_hbm, second_gain),
            ("sg", sg_hbm, sg),
            ("su", su_hbm, su),
            ("sd", sd_hbm, sd),
        )
    ):
        loads[name] = pltpu.make_async_copy(source, target, load_sem.at[number])

    def load(*names):
        for name in names:
            loads[name].start()

    def loaded(*names):
        for name in names:
            loads[name].wait()

    load("tokens", "first_gain", "fg", "fu")
    barrier = pltpu.get_barrier_semaphore()
    kv_ids = {m: {"kv": flipped(me_kv, m)} for m in partners(n_kv)}
    tp_ids = {m: {"tp": flipped(me_tp, m)} for m in partners(n_tp)}
    for ids in (kv_ids, tp_ids):
        for device in ids.values():
            pl.semaphore_signal(barrier, inc=1, device_id=device, device_id_type=MESH)
    load("fd", "lengths", "inv_freq", "attn_gain")

    started = []

    def send(slot, axis, number):
        if axis == "kv":
            ids, me, send_sem, recv_sem = kv_ids, me_kv, kv_send, kv_recv
        else:
            ids, me, send_sem, recv_sem = tp_ids, me_tp, tp_send, tp_recv
        copies = []
        for m, device in ids.items():
            copy = pltpu.make_async_remote_copy(
                src_ref=slot(me),
                dst_ref=slot(me),
                send_sem=send_sem.at[number, m - 1],
                recv_sem=recv_sem.at[number, m - 1],
                device_id=device,
                device_id_type=MESH,
            )
            copy.start()
            copies.append(copy)
        started.extend(copies)
        return copies

    def receive(copies):
        for copy in copies:
            copy.wait_recv()

    def settle(keep=0):
        while len(started) > keep:
            started.pop(0).wait_send()

    def scaled_of(stream_f, gain):
        scaled = (stream_f * gain[...].astype(F32)).astype(BF16)
        return scaled, jnp.sum(stream_f * stream_f, axis=1, keepdims=True)

    def half_step(stream_f, gain, gate, up, downw, names, mix, down, number, ready, after):
        scaled, square = scaled_of(stream_f, gain)
        high = square.astype(BF16)
        low = (square - high.astype(F32)).astype(BF16)
        loaded(names[0])
        mix[me_kv, 0, :, :units] = turned(scaled, gate[...]).astype(BF16)
        mix[me_kv, 0, :, units:] = jnp.broadcast_to(high, (seqs, pad - units))
        ready()
        sent = send(lambda i: mix.at[i, 0], "kv", number)
        loaded(names[1])
        mix[me_kv, 1, :, :units] = turned(scaled, up[...]).astype(BF16)
        mix[me_kv, 1, :, units:] = jnp.broadcast_to(low, (seqs, pad - units))
        sent = sent + send(lambda i: mix.at[i, 1], "kv", number + 1)
        after()
        loaded(names[2])
        settle(keep=len(sent))
        receive(sent)
        gate_sum = mix[0, 0].astype(F32)
        up_sum = mix[0, 1].astype(F32)
        for i in range(1, n_kv):
            gate_sum = gate_sum + mix[i, 0].astype(F32)
            up_sum = up_sum + mix[i, 1].astype(F32)
        total = gate_sum[:, units : units + 1] + up_sum[:, units : units + 1]
        row_scale = lax.rsqrt(total / width + EPSILON)
        gated = row_scale * gate_sum[:, :units]
        hidden = (gated * jax.nn.sigmoid(gated) * (row_scale * up_sum[:, :units])).astype(BF16)
        return reduced(jnp.dot(hidden, downw[...], preferred_element_type=F32), down, number // 2)

    def reduced(partial, buffer, number):
        buffer[me_tp] = partial.astype(buffer.dtype)
        sent = send(lambda i: buffer.at[i], "tp", number)
        settle(keep=len(sent))
        receive(sent)
        total = buffer[0].astype(F32)
        for i in range(1, n_tp):
            total = total + buffer[i].astype(F32)
        return total

    def ready():
        pl.semaphore_wait(barrier, n_kv + n_tp - 2)

    def load_rest():
        load("wq", "wk", "wv", "keys", "values", "lambdas", "head_gain", "wo")
        load("second_gain", "sg", "su", "sd")

    loaded("tokens", "first_gain")
    stream = tokens[...].astype(F32)
    mixed_sum = half_step(
        stream, first_gain, fg, fu, fd, ("fg", "fu", "fd"), mix1, down1, 0, ready, load_rest
    )
    first = (stream + 0.5 * mixed_sum).astype(BF16).astype(F32)

    loaded("attn_gain", "wq")
    scaled, square = scaled_of(first, attn_gain)
    span = heads * 128
    qnew[me_kv, :, :span] = jnp.dot(scaled, wq[...], preferred_element_type=F32)
    qnew[me_kv, :, span:] = jnp.broadcast_to(square, (seqs, 128))
    q_sent = send(lambda i: qnew.at[i], "kv", 4)
    loaded("wk")
    knew[me_kv] = jnp.dot(scaled, wk[...], preferred_element_type=F32)
    kv_sent = send(lambda i: knew.at[i], "kv", 5)
    loaded("wv")
    vnew[me_kv] = jnp.dot(scaled, wv[...], preferred_element_type=F32).astype(BF16)
    kv_sent = kv_sent + send(lambda i: vnew.at[i], "kv", 6)
    settle(keep=len(q_sent) + len(kv_sent))

    loaded("lengths", "inv_freq")
    lane = lax.broadcasted_iota(jnp.int32, (seqs, 128), 1)
    row = lax.broadcasted_iota(jnp.int32, (seqs, 128), 0)
    position = jnp.zeros((seqs, 128), jnp.int32)
    for b in range(seqs):
        position = jnp.where(row == b, lengths[b], position)
    angles = position.astype(F32) * inv_freq[...]
    cosine = jnp.cos(angles)
    sine = jnp.sin(angles)
    lower = lax.rem(lane, 64) < 32
    sine = jnp.where(lower, -sine, sine)
    left_half = lane < 64

    def rotated(x):
        other = jnp.where(lower, pltpu.roll(x, 96, 1), pltpu.roll(x, 32, 1))
        return (x * cosine + other * sine).astype(BF16).astype(F32)

    places = keys.shape[1] // heads
    shape = (8, keys.shape[1])
    column = lax.broadcasted_iota(jnp.int32, shape, 1)
    query_row = lax.broadcasted_iota(jnp.int32, shape, 0)
    spot = me_kv * places + lax.div(column, heads)
    spot = jnp.where(lax.rem(column, heads) == lax.div(query_row, 2), spot, 1 << 30)

    qrows[...] = jnp.zeros_like(qrows)
    loaded("keys", "values")
    receive(q_sent)
    sums = qnew[0]
    for i in range(1, n_kv):
        sums = sums + qnew[i]
    row_scale = lax.rsqrt(sums[:, span : span + 1] / width + EPSILON)
    queries = []
    for h in range(heads):
        query = rotated(row_scale * sums[:, h * 128 : (h + 1) * 128])
        queries.append(query)
        for c in range(2):
            half = left_half if c == 0 else jnp.logical_not(left_half)
            qrows[:, 2 * h + c, :] = jnp.where(half, query * 0.125, 0.0)

    scores = {}
    for step in range(seqs + AHEAD):
        if step < seqs:
            scores[step] = turned(qrows[step].astype(BF16), keys[step])
        b = step - AHEAD
        if b < 0:
            continue
        masked = jnp.where(spot < lengths[b], scores.pop(b), MASKED_SCORE)
        peak = jnp.max(masked, axis=1, keepdims=True)
        weights = jnp.exp(masked - jnp.maximum(peak, 0.5 * MASKED_SCORE))
        total = jnp.sum(weights, axis=1, keepdims=True)
        summed = jnp.dot(weights.astype(BF16), values[b], preferred_element_type=F32)
        own_part[0:rows, b, :] = summed[:rows]
        own_part[rows : 2 * rows, b, :] = jnp.broadcast_to(peak, (8, 128))[:rows]
        own_part[2 * rows : 3 * rows, b, :] = jnp.broadcast_to(total, (8, 128))[:rows]
    compact = jnp.zeros((seqs, 128), F32)
    for r in range(rows):
        compact = jnp.where(lane == r, own_part[rows + r], compact)
        compact = jnp.where(lane == 64 + r, own_part[2 * rows + r], compact)
    stat[me_kv] = compact
    stat_sent = send(lambda i: stat.at[i], "kv", 7)
    part[me_kv] = own_part[0:rows].astype(BF16)
    part_sent = send(lambda i: part.at[i], "kv", 8)
    settle(keep=len(stat_sent) + len(part_sent))

    receive(kv_sent)
    key_sum = knew[0]
    for i in range(1, n_kv):
        key_sum = key_sum + knew[i]
    own = jnp.zeros((seqs, 128), F32)
    for h in range(heads):
        fresh = rotated(row_scale * key_sum[:, h * 128 : (h + 1) * 128])
        product = queries[h] * fresh
        for c in range(2):
            half = left_half if c == 0 else jnp.logical_not(left_half)
            score = jnp.sum(jnp.where(half, product, 0.0), axis=1, keepdims=True) * 0.125
            own = jnp.where(lane == 2 * h + c, score, own)
    value_sum = vnew[0].astype(F32)
    for i in range(1, n_kv):
        value_sum = value_sum + vnew[i].astype(F32)
    fresh_value = (row_scale * value_sum).astype(BF16).astype(F32)
    loaded("wo", "lambdas", "head_gain")
    gain_out = head_gain[...].astype(F32) * OUTPUT_KEEP
    receive(stat_sent)
    stats = [stat[i] for i in range(n_kv)]
    top = own
    for s in stats:
        top = jnp.maximum(top, s)
    fresh_weight = jnp.exp(own - top)
    shares = [jnp.exp(s - top) for s in stats]
    below = fresh_weight
    for s, share in zip(stats, shares):
        below = below + pltpu.roll(s, 64, 1) * share
    fresh_weight = fresh_weight / below
    shares = [share / below for share in shares]
    receive(part_sent)
    normed = []
    for h in range(heads):
        maps = []
        for c in range(2):
            r = 2 * h + c
            above = fresh_weight[:, r : r + 1] * fresh_value[:, h * 128 : (h + 1) * 128]
            for i in range(n_kv):
                above = above + shares[i][:, r : r + 1] * part[i, r].astype(F32)
            maps.append(above)
        head = maps[0] - lambdas[h] * maps[1]
        norm = lax.rsqrt(jnp.mean(head * head, axis=1, keepdims=True) + EPSILON)
        normed.append((head * norm * gain_out).astype(BF16))
    projected = jnp.dot(
        jnp.concatenate(normed, axis=1), wo[...], preferred_element_type=F32
    )
    second = (first + reduced(projected, proj, 2)).astype(BF16).astype(F32)

    nothing = (lambda: None, lambda: None)
    loaded("second_gain")
    mixed_sum = half_step(
        second, second_gain, sg, su, sd, ("sg", "su", "sd"), mix2, down2, 2, *nothing
    )
    out_ref[...] = (second + 0.5 * mixed_sum).astype(BF16)
    settle()


def local(n_kv, n_tp, *args):
    (
        tokens,
        lengths,
        cache_keys,
        cache_values,
        lambdas,
        head_gain,
        attn_gain,
        w_query,
        w_key,
        w_value,
        w_out,
        first_gain,
        first_gate,
        first_up,
        first_down,
        second_gain,
        second_gate,
        second_up,
        second_down,
    ) = args
    seqs, cols = tokens.shape
    places, heads, wide = cache_keys.shape[1:]
    flat = (seqs, places * heads, wide)
    keys = cache_keys.reshape(flat)
    values = cache_values.reshape(flat)
    first_gate, first_up, second_gate, second_up = (
        a.T for a in (first_gate, first_up, second_gate, second_up)
    )
    units = first_gate.shape[0]
    pad = (units // 128 + 1) * 128
    span = heads * 128
    half = np.float32(ROTARY_BASE) ** (-np.arange(32, dtype=np.float32) / np.float32(32))
    inv_freq = jnp.asarray(np.tile(half.astype(np.float32), 4)[None, :])
    hbm = pl.BlockSpec(memory_space=pl.ANY)
    stay = [tokens, keys, values, w_query, w_key, w_value, w_out]
    stay += [first_gate, first_up, first_down, second_gate, second_up, second_down]
    stay += [head_gain, attn_gain, first_gain, second_gain, inv_freq]
    dma = pltpu.SemaphoreType.DMA
    return pl.pallas_call(
        functools.partial(kernel, n_kv, n_tp, cols * n_kv),
        out_shape=pltpu.VMEM((seqs, cols), BF16),
        in_specs=[hbm] * 20,
        out_specs=pl.BlockSpec(memory_space=pltpu.VMEM),
        scratch_shapes=[pltpu.VMEM(a.shape, a.dtype) for a in stay]
        + [pltpu.SMEM(a.shape, a.dtype) for a in (lengths, lambdas)]
        + [
            pltpu.VMEM((n_kv, 2, seqs, pad), BF16),
            pltpu.VMEM((n_kv, 2, seqs, pad), BF16),
            pltpu.VMEM((n_tp, seqs, cols), BF16),
            pltpu.VMEM((n_tp, seqs, cols), BF16),
            pltpu.VMEM((n_tp, seqs, cols), BF16),
            pltpu.VMEM((n_kv, seqs, span + 128), F32),
            pltpu.VMEM((n_kv, seqs, span), F32),
            pltpu.VMEM((n_kv, seqs, span), BF16),
            pltpu.VMEM((n_kv, 2 * heads, seqs, 128), BF16),
            pltpu.VMEM((n_kv, seqs, 128), F32),
            pltpu.VMEM((6 * heads, seqs, 128), F32),
            pltpu.VMEM((seqs, 8, 128), F32),
            dma((len(stay) + 2,)),
            dma((9, n_kv - 1)),
            dma((9, n_kv - 1)),
            dma((3, n_tp - 1)),
            dma((3, n_tp - 1)),
        ],
        compiler_params=pltpu.CompilerParams(
            collective_id=0, has_side_effects=True, vmem_limit_bytes=56 * 1024 * 1024
        ),
    )(
        tokens,
        lengths,
        keys,
        values,
        lambdas,
        head_gain,
        attn_gain,
        w_query,
        w_key,
        w_value,
        w_out,
        first_gain,
        first_gate,
        first_up,
        first_down,
        second_gain,
        second_gate,
        second_up,
        second_down,
        inv_freq,
    )


def solution(mesh):
    return jax.shard_map(
        functools.partial(local, mesh.shape["kv"], mesh.shape["tp"]),
        mesh=mesh,
        in_specs=(
            P(None, "kv"),
            P(),
            P(None, "kv", "tp", None),
            P(None, "kv", "tp", None),
            P("tp"),
            P(),
            P("kv"),
            P("kv", "tp"),
            P("kv", "tp"),
            P("kv", "tp"),
            P("tp", "kv"),
            P("kv"),
            P("kv", "tp"),
            P("kv", "tp"),
            P("tp", "kv"),
            P("kv"),
            P("kv", "tp"),
            P("kv", "tp"),
            P("tp", "kv"),
        ),
        out_specs=P(None, "kv"),
        check_vma=False,
    )
```
